32 devices in a mesh: ep: 16 (over z, y, core), tp: 2 (over x).
Axes of the slice: x: 2, y: 2, z: 4, core: 2. Of those that a mesh axis runs over, the one named last changes fastest.
Arguments:
- tokens: bfloat16 [256, 2048], P('ep'), may hold values from -6 to 6
- positions: int32 [256], P('ep'), may hold values from 1024 to 16383
- state: float32 [256, 4, 128, 128], P('ep', 'tp'), may hold values from -1 to 1
- mix_gain: float32 [2048], replicated, may hold values from 0.1 to 1.9
- w_query: bfloat16 [2048, 512], P(None, 'tp'), may hold values from -0.125 to 0.125
- w_key: bfloat16 [2048, 512], P(None, 'tp'), may hold values from -0.125 to 0.125
- w_value: bfloat16 [2048, 512], P(None, 'tp'), may hold values from -0.125 to 0.125
- w_out: bfloat16 [512, 2048], P('tp'), may hold values from -0.25 to 0.25
- ffn_gain: float32 [2048], replicated, may hold values from 0.1 to 1.9
- branch_gate: bfloat16 [2048], replicated, may hold values from -0.125 to 0.125
- dense_gate: bfloat16 [2048, 4096], P('tp', 'ep'), may hold values from -0.125 to 0.125
- dense_up: bfloat16 [2048, 4096], P('tp', 'ep'), may hold values from -0.125 to 0.125
- dense_down: bfloat16 [4096, 2048], P('ep', 'tp'), may hold values from -0.09375 to 0.09375
- routes: int32 [256, 6], P('ep'), may hold values from 0 to 15, all different within a row; in each aligned block of 16 rows (0 to 15, 16 to 31, ...) at most 12 rows name the same one
- route_scores: float32 [256, 6], P('ep'), may hold values from 0.05 to 1
- expert_gate: bfloat16 [16, 2048, 512], P('ep', None, 'tp'), may hold values from -0.125 to 0.125
- expert_up: bfloat16 [16, 2048, 512], P('ep', None, 'tp'), may hold values from -0.125 to 0.125
- expert_down: bfloat16 [16, 512, 2048], P('ep', 'tp'), may hold values from -0.25 to 0.25
Outputs:
- layer_out: bfloat16 [256, 2048], P('ep', 'tp')
The draws below stay inside these ranges and needn't reach their ends.
Inputs may be any that keep to these rules, and one draw needn't show every extreme that they name: `routes`: each row names 6 different experts. In each aligned block of 16 rows (the rows of one index of ep) no expert is named by more than 12 rows, a bound that some block reaches.
All inputs are finite; a program needn't handle non-finite values.
Results may differ from the reference program's by a relative error of at most 0.012.
Values may be sent and summed in bfloat16 or wider, within the bound.
No kernel may reach another device: no remote copies, remote signals or barrier semaphores. Data moves between devices by JAX's collectives and lax.ppermute only.
A program may use at most 64 MiB of HBM per device.

```python
import math
import jax
import jax.numpy as jnp
import numpy as np
from jax import lax

D = 2048
HEADS = 4
HEAD = 128
EXPERT_W = 512
DENSE = 4096
TOP = 6
SEQ_DEV = 16
BATCH = 256
EXPERTS = 16
CAP = 12
N_EP = 16
N_TP = 2


def set_ends(result, stream_key, smallest, high):
    shape = result.shape
    spot = [jax.random.randint(jax.random.fold_in(stream_key, axis), (), 0, shape[axis]) for axis in range(len(shape))]
    result = result.at[tuple(spot)].set(smallest)
    longest = shape.index(max(shape))
    spot[longest] = (spot[longest] + 1) % shape[longest]
    return result.at[tuple(spot)].set(high)


def level_of(own_key, shape, split, smallest, top_value):
    gain, own = 1.0, jax.random.fold_in(own_key, 6)
    for axis_at, blocks in split:
        heights = jnp.exp(jax.random.uniform(jax.random.fold_in(own, axis_at), (blocks,), jnp.float32, smallest / len(split), top_value / len(split)))
        gain = gain * jnp.repeat(heights, shape[axis_at] // blocks).reshape([-1 if axis == axis_at else 1 for axis in range(len(shape))])
    return gain


def routed_block(stream_key, own, number, rows, count, top, reach, skew):
    sequence = jax.random.permutation(stream_key, count)
    heavy_load, ordinary = shares(count, rows * top, reach, skew, True), shares(count, rows * top, reach, skew, False)
    places = jnp.arange(count)

    def named(tallies, turn):
        used = int((tallies > 0).sum())
        fixed = max(1, used // 4)
        shifted = fixed + (places - fixed + turn * (used - fixed)) % max(1, count - fixed)
        return jnp.zeros((count,), jnp.int32).at[sequence[jnp.where(places < fixed, places, shifted)]].set(jnp.asarray(tallies, jnp.int32))

    tallies = jnp.where(number % 4 == 0, named(heavy_load, number // 4), named(ordinary, number - number // 4 - 1))
    mixed = jax.random.permutation(jax.random.fold_in(own, 3), count)
    donor, taker = mixed[0:count // 2 * 2:2], mixed[1:count // 2 * 2:2]
    room = jnp.minimum(tallies[donor] - 1, reach - tallies[taker]) // 2
    room = jnp.where((donor == sequence[0]) | (taker == sequence[0]) | (tallies[taker] == 0), 0, jnp.maximum(room, 0))
    shifted = jax.random.randint(jax.random.fold_in(own, 4), (count // 2,), 0, 1 << 20) % (room + 1)
    tallies = tallies.at[donor].add(-shifted).at[taker].add(shifted)
    labels = jnp.searchsorted(jnp.cumsum(tallies), jnp.arange(rows * top), side="right").astype(jnp.int32)
    grid = labels.reshape(top, rows).T
    grid = grid[jax.random.permutation(jax.random.fold_in(own, 1), rows)]
    turn = jax.random.randint(jax.random.fold_in(own, 2), (rows, 1), 0, top)
    return jnp.take_along_axis(grid, (jnp.arange(top)[None, :] + turn) % top, axis=1)


def shares(amount, total, reach, slope, full):
    portions = [(1 << 20) // math.isqrt(grade ** slope) + 1 for grade in range(1, amount + 1)]
    largest = reach if full else min(reach, max(-(-total // amount), total * portions[0] // sum(portions)))
    least = 1 if total - largest >= amount - 1 else 0
    holding, rest = [largest] + [least] * (amount - 1), total - largest - least * (amount - 1)
    while rest > 0:
        candidates = [i for i in range(1, amount) if holding[i] < largest] or [i for i in range(1, amount) if holding[i] < reach]
        mass, budget = sum([portions[i] for i in candidates]), rest
        for i in candidates:
            addition = min(reach - holding[i], max(1, budget * portions[i] // mass), rest)
            holding[i] = holding[i] + addition
            rest = rest - addition
    return np.array(holding)


def noise(own_key, extent, deviation, bound, cuts=(), held_as=jnp.bfloat16):
    result = jax.random.normal(own_key, extent, jnp.float32) * deviation
    if len(cuts) > 0:
        result = level_of(own_key, extent, cuts, -0.22, 0.18) * result
    return jnp.clip(result, min=-bound, max=bound).astype(held_as)


def setup_inputs(seed: int = 0) -> dict:
    arg_keys = jax.random.split(jax.random.key(seed), 19)
    tokens = noise(arg_keys[0], (BATCH, D), 1.0, 6.0, ((0, 16),))
    positions = set_ends(jax.random.randint(arg_keys[1], (BATCH,), 1024, 16384), jax.random.fold_in(arg_keys[1], 1), 1024, 16383).astype(jnp.int32)
    state = noise(arg_keys[2], (BATCH, HEADS, HEAD, HEAD), (2 * HEAD ** -0.5), 1.0, ((0, 16), (1, 2)), jnp.float32)
    mix_gain = jnp.clip(1.0 + 0.18 * jax.random.normal(arg_keys[3], (D,), jnp.float32), 0.1, 1.9)
    w_query = noise(arg_keys[4], (D, HEADS * HEAD), D ** -0.5, 0.125, ((1, 2),))
    w_key = noise(arg_keys[5], (D, HEADS * HEAD), D ** -0.5, 0.125, ((1, 2),))
    w_value = noise(arg_keys[6], (D, HEADS * HEAD), D ** -0.5, 0.125, ((1, 2),))
    w_out = noise(arg_keys[7], (HEADS * HEAD, D), (HEADS * HEAD) ** -0.5, 0.25, ((0, 2),))
    ffn_gain = jnp.clip(1.0 + 0.18 * jax.random.normal(arg_keys[8], (D,), jnp.float32), 0.1, 1.9)
    branch_gate = noise(arg_keys[9], (D,), D ** -0.5, 0.125)
    dense_gate = noise(arg_keys[10], (D, DENSE), D ** -0.5, 0.125, ((0, 2), (1, 16)))
    dense_up = noise(arg_keys[11], (D, DENSE), D ** -0.5, 0.125, ((0, 2), (1, 16)))
    dense_down = noise(arg_keys[12], (DENSE, D), DENSE ** -0.5, 0.09375, ((0, 16), (1, 2)))
    routes_keys = jax.random.split(jax.random.fold_in(arg_keys[13], 1), BATCH // SEQ_DEV)
    routes_turns = jax.random.permutation(jax.random.fold_in(arg_keys[13], 3), BATCH // SEQ_DEV)
    routes = jax.vmap(lambda own, number: routed_block(jax.random.fold_in(arg_keys[13], 2), own, number, SEQ_DEV, EXPERTS, TOP, CAP, 2))(routes_keys, routes_turns).reshape((BATCH, TOP))
    route_scores = jnp.clip(jnp.exp(math.log(1.0) - 2.9957323 * jax.random.uniform(arg_keys[14], (BATCH, TOP), jnp.float32) ** level_of(arg_keys[14], (BATCH, TOP), ((0, 16),), -0.2, 0.2)), 0.05, 1.0)
    expert_gate = noise(arg_keys[15], (EXPERTS, D, EXPERT_W), D ** -0.5, 0.125, ((0, 16), (2, 2)))
    expert_up = noise(arg_keys[16], (EXPERTS, D, EXPERT_W), D ** -0.5, 0.125, ((0, 16), (2, 2)))
    expert_down = noise(arg_keys[17], (EXPERTS, EXPERT_W, D), EXPERT_W ** -0.5, 0.25, ((0, 16), (1, 2)))
    return {"tokens": tokens, "positions": positions, "state": state, "mix_gain": mix_gain, "w_query": w_query, "w_key": w_key, "w_value": w_value, "w_out": w_out, "ffn_gain": ffn_gain, "branch_gate": branch_gate, "dense_gate": dense_gate, "dense_up": dense_up, "dense_down": dense_down, "routes": routes, "route_scores": route_scores, "expert_gate": expert_gate, "expert_up": expert_up, "expert_down": expert_down}


EPS = 1e-06

def normalize(inputs, scale_vec):
    values = inputs.astype(jnp.float32)
    return values * lax.rsqrt(lax.optimization_barrier(jnp.mean(values * values, axis=-1, keepdims=True)) + EPS) * scale_vec

def rotate(vectors, where):
    half = vectors.shape[-1] // 2
    inverse = 1.0 / 10000.0 ** jnp.linspace(0.0, 1.0, half, dtype=jnp.float32)
    angle = where.astype(jnp.float32)[:, None] * inverse[None, :]
    cosine = jnp.cos(angle)[:, None, :]
    sine = jnp.sin(angle)[:, None, :]
    first = vectors[..., :half]
    second = vectors[..., half:]
    return jnp.concatenate([first * cosine - second * sine, second * cosine + first * sine], axis=-1)

def blocked_sum(left, right, blocks):
    inner = left.shape[1] // blocks
    total = jnp.zeros((left.shape[0], right.shape[1]), jnp.float32)
    for block in range(blocks):
        partial_value = jnp.dot(left[:, block * inner:(block + 1) * inner], right[block * inner:(block + 1) * inner], preferred_element_type=jnp.float32)
        rounded = lax.optimization_barrier(partial_value.astype(jnp.bfloat16))
        total = total + rounded.astype(jnp.float32)
    return total

def reference(tokens, positions, state, mix_gain, w_query, w_key, w_value, w_out, ffn_gain, branch_gate, dense_gate, dense_up, dense_down, routes, route_scores, expert_gate, expert_up, expert_down):
    normed = normalize(tokens, mix_gain).astype(jnp.bfloat16)
    query_vec = jnp.dot(normed, w_query, preferred_element_type=jnp.float32).reshape(BATCH, HEADS, HEAD)
    key_vec = jnp.dot(normed, w_key, preferred_element_type=jnp.float32).reshape(BATCH, HEADS, HEAD)
    value_vec = jnp.dot(normed, w_value, preferred_element_type=jnp.float32).reshape(BATCH, HEADS, HEAD)
    query_vec = rotate(query_vec, positions)
    key_vec = rotate(key_vec, positions) * HEAD ** (-0.5)
    head_index = jnp.arange(HEADS, dtype=jnp.float32)
    decay_rate = 1.0 - 2.0 ** (-5.0 - 5.0 * head_index / (HEADS - 1))
    new_state = decay_rate[None, :, None, None] * state + key_vec[:, :, :, None] * value_vec[:, :, None, :]
    retrieved = jnp.einsum('bhd,bhe->bhe', query_vec, jnp.zeros_like(value_vec)) + jnp.einsum('bhd,bhde->bhe', query_vec, new_state, precision=lax.Precision.HIGHEST)
    retrieved = retrieved * lax.rsqrt(lax.optimization_barrier(jnp.mean(retrieved * retrieved, axis=-1, keepdims=True)) + EPS)
    retrieved = retrieved.reshape(BATCH, HEADS * HEAD).astype(jnp.bfloat16)
    mixer_out = blocked_sum(retrieved, w_out, N_TP)
    after_mix = tokens.astype(jnp.float32) + mixer_out
    ffn_in = normalize(after_mix, ffn_gain).astype(jnp.bfloat16)
    per_block = SEQ_DEV * TOP
    chosen = routes.reshape(N_EP, per_block)
    marks = (chosen[:, :, None] == jnp.arange(EXPERTS, dtype=jnp.int32)[None, None, :]).astype(jnp.int32)
    ranking = lax.optimization_barrier(jnp.sum((jnp.cumsum(marks, axis=1) - marks) * marks, axis=2)).astype(jnp.int32)
    source = jnp.broadcast_to(jnp.arange(N_EP, dtype=jnp.int32)[:, None], (N_EP, per_block))
    token_of = (jnp.arange(BATCH * TOP, dtype=jnp.int32) // TOP).reshape(N_EP, per_block)
    buffer = jnp.zeros((EXPERTS, N_EP, CAP, D), jnp.bfloat16).at[chosen, source, ranking].set(ffn_in[token_of])

    def one_expert(pieces):
        rows_in, gate_mat, up_mat, down_mat = pieces
        flat_rows = rows_in.reshape(N_EP * CAP, D)
        gate_pre = jnp.dot(flat_rows, gate_mat, preferred_element_type=jnp.float32)
        up_pre = jnp.dot(flat_rows, up_mat, preferred_element_type=jnp.float32)
        hidden = (jax.nn.silu(gate_pre) * up_pre).astype(jnp.bfloat16)
        return blocked_sum(hidden, down_mat, N_TP).astype(jnp.bfloat16).reshape(N_EP, CAP, D)
    results = lax.map(one_expert, (buffer, expert_gate, expert_up, expert_down))
    picked = results[chosen, source, ranking].reshape(BATCH, TOP, D).astype(jnp.float32)
    route_weights = route_scores / lax.optimization_barrier(jnp.sum(route_scores, axis=1, keepdims=True))
    experts_out = lax.optimization_barrier(jnp.sum(route_weights[:, :, None] * picked, axis=1))
    pre_gate = blocked_sum(ffn_in, dense_gate, N_TP)
    pre_up = blocked_sum(ffn_in, dense_up, N_TP)
    dense_hidden = (jax.nn.silu(pre_gate) * pre_up).astype(jnp.bfloat16)
    dense_out = jnp.dot(dense_hidden, dense_down, preferred_element_type=jnp.float32)
    branch_weight = jax.nn.sigmoid(jnp.dot(ffn_in, branch_gate, preferred_element_type=jnp.float32))
    return (after_mix + experts_out + branch_weight[:, None] * dense_out).astype(jnp.bfloat16)
```

```python
import jax
import jax.numpy as jnp
from jax import lax
from jax.experimental import pallas as pl
from jax.experimental.pallas import tpu as pltpu
from jax.sharding import PartitionSpec as P

EPS = 1e-06
LANES = 128
F32 = jnp.float32
BF16 = jnp.bfloat16


def dot(a, b):
    return jnp.dot(a, b, preferred_element_type=F32)


def rotary_tables(positions, head_dim):
    half = head_dim // 2
    inverse = 1.0 / 10000.0 ** jnp.linspace(0.0, 1.0, half, dtype=F32)
    angle = positions.astype(F32)[:, None] * inverse[None, :]
    cosine = jnp.cos(angle)
    sine = jnp.sin(angle)
    return jnp.concatenate([cosine, cosine], 1), jnp.concatenate([-sine, sine], 1)


def mixer_kernel(tok, gain, cos, sin, decay, wq, wk, wv, st, wo, out, q_buf, k_buf, v_buf, s_buf, o_buf, sems):
    copies = [
        pltpu.make_async_copy(src, dst, sems.at[i])
        for i, (src, dst) in enumerate(
            [(wq, q_buf), (wk, k_buf), (wv, v_buf), (st, s_buf), (wo, o_buf)]
        )
    ]
    for copy in copies:
        copy.start()
    rows, heads, head_dim = s_buf.shape[0], s_buf.shape[1], s_buf.shape[2]
    values = tok[...].astype(F32)
    scale = lax.rsqrt(jnp.mean(values * values, axis=-1, keepdims=True) + EPS)
    normed = (values * scale * gain[...]).astype(BF16)
    copies[0].wait()
    query = dot(normed, q_buf[...])
    copies[1].wait()
    key = dot(normed, k_buf[...])
    copies[2].wait()
    value = dot(normed, v_buf[...])
    cosine, sine = cos[...], sin[...]
    half = head_dim // 2
    copies[3].wait()
    parts = []
    for h in range(heads):
        cols = slice(h * head_dim, (h + 1) * head_dim)
        q = query[:, cols]
        k = key[:, cols]
        q = q * cosine + pltpu.roll(q, half, 1) * sine
        k = (k * cosine + pltpu.roll(k, half, 1) * sine) * head_dim ** (-0.5)
        turned = q.T
        old = jnp.concatenate(
            [
                jnp.sum(turned[:, b : b + 1] * s_buf[b, h], axis=0, keepdims=True)
                for b in range(rows)
            ],
            axis=0,
        )
        got = decay[:, cols] * old + jnp.sum(q * k, axis=-1, keepdims=True) * value[:, cols]
        got = got * lax.rsqrt(jnp.mean(got * got, axis=-1, keepdims=True) + EPS)
        parts.append(got.astype(BF16))
    retrieved = parts[0] if heads == 1 else jnp.concatenate(parts, axis=1)
    copies[4].wait()
    out[...] = dot(retrieved, o_buf[...]).astype(BF16)


def mixer(tokens, gain, cos, sin, decay, wq, wk, wv, state, wo):
    vmem = pl.BlockSpec(memory_space=pltpu.VMEM)
    hbm = pl.BlockSpec(memory_space=pl.ANY)
    return pl.pallas_call(
        mixer_kernel,
        out_shape=jax.ShapeDtypeStruct(tokens.shape, BF16),
        in_specs=[vmem] * 5 + [hbm] * 5,
        out_specs=vmem,
        scratch_shapes=[pltpu.VMEM(a.shape, a.dtype) for a in (wq, wk, wv, state, wo)]
        + [pltpu.SemaphoreType.DMA((5,))],
        name="mixer",
    )(tokens, gain, cos, sin, decay, wq, wk, wv, state, wo)


def norm_kernel(fanout, tok, gain, gate, meta, *refs):
    parts, (rows_out, mix_out) = refs[:-2], refs[-2:]
    width = tok.shape[1]
    mixed = parts[0][...].astype(F32)
    for part in parts[1:]:
        mixed = mixed + part[...].astype(F32)
    after = tok[...].astype(F32) + mixed
    mix_out[...] = after
    scale = lax.rsqrt(jnp.mean(after * after, axis=-1, keepdims=True) + EPS)
    ffn = (after * scale * gain[...]).astype(BF16)
    rows_out[:, :width] = ffn
    logit = jnp.sum(ffn.astype(F32) * gate[...].astype(F32), axis=-1, keepdims=True)
    branch = 1.0 / (1.0 + jnp.exp(-logit))
    high = branch.astype(BF16).astype(F32)
    low = branch - high
    info = meta[...].astype(F32)
    lane = lax.broadcasted_iota(jnp.int32, info.shape, 1)
    info = jnp.where(lane == 3 * fanout, high, info)
    info = jnp.where(lane == 3 * fanout + 1, low, info)
    rows_out[:, width:] = info.astype(BF16)


def norm_rows(fanout, tokens, gain, gate, meta, parts):
    vmem = pl.BlockSpec(memory_space=pltpu.VMEM)
    rows, width = tokens.shape
    return pl.pallas_call(
        lambda *refs: norm_kernel(fanout, *refs),
        out_shape=(
            jax.ShapeDtypeStruct((rows, width + LANES), BF16),
            jax.ShapeDtypeStruct((rows, width), F32),
        ),
        in_specs=[vmem] * (4 + len(parts)),
        out_specs=(vmem, vmem),
        name="norm",
    )(tokens, gain, gate, meta, *parts)


def silu(v):
    return v / (1.0 + jnp.exp(-v))


def branch_kernel(tp_count, fanout, place, near, far, eg, eu, ed, *refs):
    pieces = refs[: 2 * tp_count]
    near_out, far_out = refs[2 * tp_count : 2 * tp_count + 2]
    bufs = refs[2 * tp_count + 2 : -1]
    sems = refs[-1]
    sources = [eg, eu, *pieces[:tp_count], ed, *pieces[tp_count:]]
    copies = [
        pltpu.make_async_copy(src, dst, sems.at[i])
        for i, (src, dst) in enumerate(zip(sources, bufs))
    ]
    for copy in copies:
        copy.start()
    eg_buf, eu_buf = bufs[0], bufs[1]
    dg_bufs = bufs[2 : 2 + tp_count]
    ed_buf = bufs[2 + tp_count]
    dd_bufs = bufs[3 + tp_count :]
    width = eg_buf.shape[1]
    block = width // tp_count
    units = dd_bufs[0].shape[0]
    per_device = eg_buf.shape[0]
    ep_index = place[0]
    tp_index = place[1]
    spots = [lax.rem(tp_index - t + tp_count, tp_count) * block for t in range(tp_count)]
    spots = [pl.multiple_of(s, LANES) for s in spots]
    rows = near.shape[0]
    step = min(rows, 256)
    for copy in copies:
        copy.wait()

    def work(src, dst, start):
        at = pl.ds(start, step)
        info = src[at, width:].astype(F32)
        lane = lax.broadcasted_iota(jnp.int32, info.shape, 1)
        high = pltpu.roll(info, LANES - fanout, 1)
        low = pltpu.roll(info, LANES - 2 * fanout, 1)
        branch = jnp.sum(
            jnp.where((lane >= 3 * fanout) & (lane < 3 * fanout + 2), info, 0.0),
            axis=1,
            keepdims=True,
        )
        x = src[at, :width]
        hidden = []
        for k in range(per_device):
            own = (ep_index * per_device + k).astype(F32)
            weight = jnp.sum(
                jnp.where((lane < fanout) & (info == own), high + low, 0.0), axis=1, keepdims=True
            )
            hidden.append(
                (silu(dot(x, eg_buf[k])) * dot(x, eu_buf[k]) * weight).astype(BF16)
            )
        both = dot(src[at, pl.ds(spots[0], block)], dg_bufs[0][...])
        for t in range(1, tp_count):
            both = both + dot(src[at, pl.ds(spots[t], block)], dg_bufs[t][...])
        dense = (silu(both[:, :units]) * both[:, units:] * branch).astype(BF16)
        for t in range(tp_count):
            total = dot(dense, dd_bufs[t][...])
            for k in range(per_device):
                total = total + dot(hidden[k], ed_buf[k, :, pl.ds(spots[t], block)])
            dst[t, at, :] = total.astype(BF16)

    for src, dst in ((far, far_out), (near, near_out)):
        if rows == step:
            work(src, dst, 0)
        else:

            def body(i, carry, src=src, dst=dst):
                work(src, dst, pl.multiple_of(i * step, step))
                return carry

            lax.fori_loop(0, rows // step, body, 0)


def branches(fanout, place, near, far, eg, eu, ed, gate_pieces, down_pieces):
    vmem = pl.BlockSpec(memory_space=pltpu.VMEM)
    hbm = pl.BlockSpec(memory_space=pl.ANY)
    tp_count = len(gate_pieces)
    width = eg.shape[1]
    shape = jax.ShapeDtypeStruct((tp_count, near.shape[0], width // tp_count), BF16)
    order = [eg, eu, *gate_pieces, ed, *down_pieces]
    return pl.pallas_call(
        lambda *refs: branch_kernel(tp_count, fanout, *refs),
        out_shape=(shape, shape),
        in_specs=[pl.BlockSpec(memory_space=pltpu.SMEM), vmem, vmem]
        + [hbm] * (3 + 2 * tp_count),
        out_specs=(vmem, vmem),
        scratch_shapes=[pltpu.VMEM(a.shape, a.dtype) for a in order]
        + [pltpu.SemaphoreType.DMA((len(order),))],
        name="branches",
    )(place, near, far, eg, eu, ed, *gate_pieces, *down_pieces)


def on_device(
    tokens,
    positions,
    state,
    mix_gain,
    w_query,
    w_key,
    w_value,
    w_out,
    ffn_gain,
    branch_gate,
    dense_gate,
    dense_up,
    dense_down,
    routes,
    route_scores,
    expert_gate,
    expert_up,
    expert_down,
):
    sequences, width = tokens.shape
    tp_count = lax.axis_size("tp")
    ep_count = lax.axis_size("ep")
    tp_index = lax.axis_index("tp")
    ep_index = lax.axis_index("ep")
    local_heads, head_dim = state.shape[1], state.shape[2]
    fanout = routes.shape[1]
    block = width // tp_count
    cores = 2 if ep_count % 2 == 0 else 1
    chips = ep_count // cores
    y_count = 1
    while chips % (y_count * 2) == 0 and (y_count * 2) ** 2 <= chips:
        y_count *= 2
    z_count = chips // y_count

    def send(x, dz=0, dy=0, dc=0, dx=0):
        pairs = []
        for z in range(z_count):
            for y in range(y_count):
                for c in range(cores):
                    for q in range(tp_count):
                        src = ((z * y_count + y) * cores + c) * tp_count + q
                        to_z, to_y = (z + dz) % z_count, (y + dy) % y_count
                        to_c, to_q = (c + dc) % cores, (q + dx) % tp_count
                        dst = ((to_z * y_count + to_y) * cores + to_c) * tp_count + to_q
                        pairs.append((src, dst))
        return lax.ppermute(x, ("ep", "tp"), pairs)

    cos, sin = rotary_tables(positions, head_dim)
    head_index = (tp_index * local_heads + jnp.arange(local_heads, dtype=jnp.int32)).astype(F32)
    decay = 1.0 - 2.0 ** (-5.0 - 5.0 * head_index / (local_heads * tp_count - 1))
    decay = jnp.repeat(decay, head_dim)[None, :]
    partial_out = mixer(
        tokens, mix_gain[None, :], cos, sin, decay, w_query, w_key, w_value, state, w_out
    )
    parts = [partial_out] + [send(partial_out, dx=s) for s in range(1, tp_count)]

    route_weights = route_scores / jnp.sum(route_scores, axis=1, keepdims=True)
    high = lax.reduce_precision(route_weights, 8, 7)
    low = route_weights - high
    meta = jnp.concatenate([routes.astype(F32), high, low], axis=1)
    meta = jnp.pad(meta, ((0, 0), (0, LANES - meta.shape[1]))).astype(BF16)
    payload, after_mix = norm_rows(
        fanout, tokens, ffn_gain[None, :], branch_gate[None, :], meta, parts
    )

    units = dense_gate.shape[1] // tp_count

    def gate_piece(index):
        at = lax.rem(index, tp_count) * units
        return jnp.concatenate(
            [
                lax.dynamic_slice_in_dim(dense_gate, at, units, 1),
                lax.dynamic_slice_in_dim(dense_up, at, units, 1),
            ],
            axis=1,
        )

    def down_piece(index):
        return lax.dynamic_slice_in_dim(dense_down, lax.rem(index, tp_count) * units, units, 0)

    gate_pieces = [gate_piece(tp_index)]
    down_pieces = [down_piece(tp_index)]
    for s in range(1, tp_count):
        there_gate, there_down, _ = lax.optimization_barrier(
            (gate_piece(tp_index + s), down_piece(tp_index + s), parts[s])
        )
        gate_pieces.append(send(there_gate, dx=s))
        down_pieces.append(send(there_down, dx=s))

    rows = jnp.concatenate([payload] + [send(payload, dz=s) for s in range(1, z_count)], axis=0)
    rows = jnp.concatenate([rows] + [send(rows, dy=s) for s in range(1, y_count)], axis=0)
    if cores == 2:
        far = send(rows, dc=1)
    else:
        far = rows
    place = jnp.stack([ep_index, tp_index]).astype(jnp.int32)
    near_sum, far_sum = branches(
        fanout, place, rows, far, expert_gate, expert_up, expert_down, gate_pieces, down_pieces
    )

    total = near_sum.astype(F32)
    if cores == 2:
        total = total + send(far_sum, dc=1).astype(F32)
    total = total.reshape(tp_count, y_count, z_count * sequences, block)
    narrow = total.astype(BF16)
    summed = total[0, 0]
    for t in range(tp_count):
        for y in range(y_count):
            if (t, y) != (0, 0):
                summed = summed + send(narrow[t, y], dx=-t, dy=-y).astype(F32)
    summed = summed.reshape(z_count, sequences, block)
    narrow = summed.astype(BF16)
    result = lax.dynamic_slice_in_dim(after_mix, tp_index * block, block, 1) + summed[0]
    for z in range(1, z_count):
        result = result + send(narrow[z], dz=-z).astype(F32)
    return result.astype(BF16)


def solution(mesh):
    placed = (
        P("ep", None),
        P("ep"),
        P("ep", "tp", None, None),
        P(),
        P(None, "tp"),
        P(None, "tp"),
        P(None, "tp"),
        P("tp", None),
        P(),
        P(),
        P("tp", "ep"),
        P("tp", "ep"),
        P("ep", "tp"),
        P("ep", None),
        P("ep", None),
        P("ep", None, "tp"),
        P("ep", None, "tp"),
        P("ep", "tp", None),
    )
    return jax.shard_map(
        on_device, mesh=mesh, in_specs=placed, out_specs=P("ep", "tp"), check_vma=False
    )
```

```python
import jax
import jax.numpy as jnp
import numpy as np
from jax import lax
from jax.experimental import pallas as pl
from jax.experimental.pallas import tpu as pltpu
from jax.sharding import PartitionSpec as P

EPS = 1e-06
LANES = 128
F32 = jnp.float32
BF16 = jnp.bfloat16


def dot(a, b):
    return jnp.dot(a, b, preferred_element_type=F32)


def frequencies(head_dim):
    half = head_dim // 2
    inverse = 1.0 / 10000.0 ** np.linspace(0.0, 1.0, half)
    return jnp.asarray(np.concatenate([inverse, inverse])[None, :], F32)


def turns(angle):
    whole = jnp.round(angle * (0.5 / np.pi))
    first = 6.28125
    second = float(np.float32(2 * np.pi - first).astype(jnp.bfloat16))
    third = 2 * np.pi - first - second
    rest = ((angle - whole * first) - whole * second) - whole * third
    return jnp.cos(rest), jnp.sin(rest)


def mixer_kernel(tok, gain, where, freq, wq, wk, wv, st, wo, out, q_buf, k_buf, v_buf, s_buf, o_buf, sems):
    copies = [
        pltpu.make_async_copy(src, dst, sems.at[i])
        for i, (src, dst) in enumerate(
            [(wq, q_buf), (wk, k_buf), (wv, v_buf), (st, s_buf), (wo, o_buf)]
        )
    ]
    for copy in copies:
        copy.start()
    rows, heads, head_dim = s_buf.shape[0], s_buf.shape[1], s_buf.shape[2]
    values = tok[...].astype(F32)
    scale = lax.rsqrt(jnp.mean(values * values, axis=-1, keepdims=True) + EPS)
    normed = (values * scale * gain[...]).astype(BF16)
    copies[0].wait()
    query = dot(normed, q_buf[...])
    copies[1].wait()
    key = dot(normed, k_buf[...])
    copies[2].wait()
    value = dot(normed, v_buf[...])
    half = head_dim // 2
    square = (rows, rows)
    diagonal = lax.broadcasted_iota(jnp.int32, square, 0) == lax.broadcasted_iota(
        jnp.int32, square, 1
    )
    spread = jnp.broadcast_to(where[...].astype(F32), square)
    at = jnp.sum(jnp.where(diagonal, spread, 0.0), axis=1, keepdims=True)
    cosine, sine = turns(at * freq[...])
    sine = jnp.where(lax.broadcasted_iota(jnp.int32, sine.shape, 1) < half, -sine, sine)
    all_heads = heads * lax.axis_size("tp")
    first_head = lax.axis_index("tp") * heads
    copies[3].wait()
    parts = []
    for h in range(heads):
        cols = slice(h * head_dim, (h + 1) * head_dim)
        q = query[:, cols]
        k = key[:, cols]
        q = q * cosine + pltpu.roll(q, half, 1) * sine
        k = (k * cosine + pltpu.roll(k, half, 1) * sine) * head_dim ** (-0.5)
        turned = q.T
        old = jnp.concatenate(
            [
                jnp.sum(turned[:, b : b + 1] * s_buf[b, h], axis=0, keepdims=True)
                for b in range(rows)
            ],
            axis=0,
        )
        number = jnp.full((1, head_dim), first_head + h, jnp.int32).astype(F32)
        decay = 1.0 - jnp.exp2(-5.0 - 5.0 * number / (all_heads - 1))
        got = decay * old + jnp.sum(q * k, axis=-1, keepdims=True) * value[:, cols]
        got = got * lax.rsqrt(jnp.mean(got * got, axis=-1, keepdims=True) + EPS)
        parts.append(got.astype(BF16))
    retrieved = parts[0] if heads == 1 else jnp.concatenate(parts, axis=1)
    copies[4].wait()
    out[...] = dot(retrieved, o_buf[...]).astype(BF16)


def mixer(tokens, gain, positions, freq, wq, wk, wv, state, wo):
    vmem = pl.BlockSpec(memory_space=pltpu.VMEM)
    hbm = pl.BlockSpec(memory_space=pl.ANY)
    return pl.pallas_call(
        mixer_kernel,
        out_shape=jax.ShapeDtypeStruct(tokens.shape, BF16),
        in_specs=[vmem] * 4 + [hbm] * 5,
        out_specs=vmem,
        scratch_shapes=[pltpu.VMEM(a.shape, a.dtype) for a in (wq, wk, wv, state, wo)]
        + [pltpu.SemaphoreType.DMA((5,))],
        name="mixer",
    )(tokens, gain, positions, freq, wq, wk, wv, state, wo)


def norm_kernel(fanout, tok, gain, gate, meta, *refs):
    parts, (rows_out, mix_out) = refs[:-2], refs[-2:]
    width = tok.shape[1]
    mixed = parts[0][...].astype(F32)
    for part in parts[1:]:
        mixed = mixed + part[...].astype(F32)
    after = tok[...].astype(F32) + mixed
    mix_out[...] = after
    scale = lax.rsqrt(jnp.mean(after * after, axis=-1, keepdims=True) + EPS)
    ffn = (after * scale * gain[...]).astype(BF16)
    rows_out[:, :width] = ffn
    logit = jnp.sum(ffn.astype(F32) * gate[...].astype(F32), axis=-1, keepdims=True)
    branch = 1.0 / (1.0 + jnp.exp(-logit))
    high = branch.astype(BF16).astype(F32)
    low = branch - high
    info = meta[...].astype(F32)
    lane = lax.broadcasted_iota(jnp.int32, info.shape, 1)
    info = jnp.where(lane == 3 * fanout, high, info)
    info = jnp.where(lane == 3 * fanout + 1, low, info)
    rows_out[:, width:] = info.astype(BF16)


def norm_rows(fanout, tokens, gain, gate, meta, parts):
    vmem = pl.BlockSpec(memory_space=pltpu.VMEM)
    rows, width = tokens.shape
    return pl.pallas_call(
        lambda *refs: norm_kernel(fanout, *refs),
        out_shape=(
            jax.ShapeDtypeStruct((rows, width + LANES), BF16),
            jax.ShapeDtypeStruct((rows, width), F32),
        ),
        in_specs=[vmem] * (4 + len(parts)),
        out_specs=(vmem, vmem),
        name="norm",
    )(tokens, gain, gate, meta, *parts)


def silu(v):
    return v / (1.0 + jnp.exp(-v))


def branch_kernel(tp_count, fanout, near, far, eg, eu, ed, *refs):
    pieces = refs[: 2 * tp_count]
    near_out, far_out = refs[2 * tp_count : 2 * tp_count + 2]
    bufs = refs[2 * tp_count + 2 : -1]
    sems = refs[-1]
    sources = [eg, eu, *pieces[:tp_count], ed, *pieces[tp_count:]]
    copies = [
        pltpu.make_async_copy(src, dst, sems.at[i])
        for i, (src, dst) in enumerate(zip(sources, bufs))
    ]
    for copy in copies:
        copy.start()
    eg_buf, eu_buf = bufs[0], bufs[1]
    dg_bufs = bufs[2 : 2 + tp_count]
    ed_buf = bufs[2 + tp_count]
    dd_bufs = bufs[3 + tp_count :]
    width = eg_buf.shape[1]
    block = width // tp_count
    units = dd_bufs[0].shape[0]
    per_device = eg_buf.shape[0]
    ep_index = lax.axis_index("ep")
    tp_index = lax.axis_index("tp")
    spots = [lax.rem(tp_index - t + tp_count, tp_count) * block for t in range(tp_count)]
    spots = [pl.multiple_of(s, LANES) for s in spots]
    rows = near.shape[0]
    step = min(rows, 256)
    held = list(copies)

    def need(count):
        while len(copies) - len(held) < count:
            held.pop(0).wait()

    if rows != step:
        need(len(copies))

    def work(src, dst, start):
        at = pl.ds(start, step)
        info = src[at, width:].astype(F32)
        lane = lax.broadcasted_iota(jnp.int32, info.shape, 1)
        high = pltpu.roll(info, LANES - fanout, 1)
        low = pltpu.roll(info, LANES - 2 * fanout, 1)
        branch = jnp.sum(
            jnp.where((lane >= 3 * fanout) & (lane < 3 * fanout + 2), info, 0.0),
            axis=1,
            keepdims=True,
        )
        x = src[at, :width]
        hidden = []
        for k in range(per_device):
            own = (ep_index * per_device + k).astype(F32)
            weight = jnp.sum(
                jnp.where((lane < fanout) & (info == own), high + low, 0.0), axis=1, keepdims=True
            )
            need(1)
            gate = dot(x, eg_buf[k])
            need(2)
            hidden.append((silu(gate) * dot(x, eu_buf[k]) * weight).astype(BF16))
        need(2 + tp_count)
        both = dot(src[at, pl.ds(spots[0], block)], dg_bufs[0][...])
        for t in range(1, tp_count):
            both = both + dot(src[at, pl.ds(spots[t], block)], dg_bufs[t][...])
        dense = (silu(both[:, :units]) * both[:, units:] * branch).astype(BF16)
        need(len(copies))
        for t in range(tp_count):
            total = dot(dense, dd_bufs[t][...])
            for k in range(per_device):
                total = total + dot(hidden[k], ed_buf[k, :, pl.ds(spots[t], block)])
            dst[t, at, :] = total.astype(BF16)

    for src, dst in ((far, far_out), (near, near_out)):
        if rows == step:
            work(src, dst, 0)
        else:

            def body(i, carry, src=src, dst=dst):
                work(src, dst, pl.multiple_of(i * step, step))
                return carry

            lax.fori_loop(0, rows // step, body, 0)


def branches(fanout, near, far, eg, eu, ed, gate_pieces, down_pieces):
    vmem = pl.BlockSpec(memory_space=pltpu.VMEM)
    hbm = pl.BlockSpec(memory_space=pl.ANY)
    tp_count = len(gate_pieces)
    width = eg.shape[1]
    shape = jax.ShapeDtypeStruct((tp_count, near.shape[0], width // tp_count), BF16)
    order = [eg, eu, *gate_pieces, ed, *down_pieces]
    return pl.pallas_call(
        lambda *refs: branch_kernel(tp_count, fanout, *refs),
        out_shape=(shape, shape),
        in_specs=[vmem, vmem]
        + [hbm] * (3 + 2 * tp_count),
        out_specs=(vmem, vmem),
        scratch_shapes=[pltpu.VMEM(a.shape, a.dtype) for a in order]
        + [pltpu.SemaphoreType.DMA((len(order),))],
        name="branches",
    )(near, far, eg, eu, ed, *gate_pieces, *down_pieces)


def on_device(
    tokens,
    positions,
    state,
    mix_gain,
    w_query,
    w_key,
    w_value,
    w_out,
    ffn_gain,
    branch_gate,
    dense_gate,
    dense_up,
    dense_down,
    routes,
    route_scores,
    expert_gate,
    expert_up,
    expert_down,
):
    sequences, width = tokens.shape
    tp_count = lax.axis_size("tp")
    ep_count = lax.axis_size("ep")
    tp_index = lax.axis_index("tp")
    fanout = routes.shape[1]
    block = width // tp_count
    cores = 2 if ep_count % 2 == 0 else 1
    chips = ep_count // cores
    y_count = 1
    while chips % (y_count * 2) == 0 and (y_count * 2) ** 2 <= chips:
        y_count *= 2
    z_count = chips // y_count

    def send(x, dz=0, dy=0, dc=0, dx=0):
        pairs = []
        for z in range(z_count):
            for y in range(y_count):
                for c in range(cores):
                    for q in range(tp_count):
                        src = ((z * y_count + y) * cores + c) * tp_count + q
                        to_z, to_y = (z + dz) % z_count, (y + dy) % y_count
                        to_c, to_q = (c + dc) % cores, (q + dx) % tp_count
                        dst = ((to_z * y_count + to_y) * cores + to_c) * tp_count + to_q
                        pairs.append((src, dst))
        return lax.ppermute(x, ("ep", "tp"), pairs)

    partial_out = mixer(
        tokens,
        mix_gain[None, :],
        positions[None, :],
        frequencies(state.shape[2]),
        w_query,
        w_key,
        w_value,
        state,
        w_out,
    )
    parts = [partial_out] + [send(partial_out, dx=s) for s in range(1, tp_count)]

    route_weights = route_scores / jnp.sum(route_scores, axis=1, keepdims=True)
    high = lax.reduce_precision(route_weights, 8, 7)
    low = route_weights - high
    meta = jnp.concatenate([routes.astype(F32), high, low], axis=1)
    meta = jnp.pad(meta, ((0, 0), (0, LANES - meta.shape[1]))).astype(BF16)
    payload, after_mix = norm_rows(
        fanout, tokens, ffn_gain[None, :], branch_gate[None, :], meta, parts
    )

    units = dense_gate.shape[1] // tp_count

    def gate_piece(index):
        at = lax.rem(index, tp_count) * units
        return jnp.concatenate(
            [
                lax.dynamic_slice_in_dim(dense_gate, at, units, 1),
                lax.dynamic_slice_in_dim(dense_up, at, units, 1),
            ],
            axis=1,
        )

    def down_piece(index):
        return lax.dynamic_slice_in_dim(dense_down, lax.rem(index, tp_count) * units, units, 0)

    gate_pieces = [gate_piece(tp_index)]
    down_pieces = [down_piece(tp_index)]
    for s in range(1, tp_count):
        there_gate, there_down, _ = lax.optimization_barrier(
            (gate_piece(tp_index + s), down_piece(tp_index + s), parts[s])
        )
        gate_pieces.append(send(there_gate, dx=s))
        down_pieces.append(send(there_down, dx=s))

    rows = jnp.concatenate([payload] + [send(payload, dz=s) for s in range(1, z_count)], axis=0)
    rows = jnp.concatenate([rows] + [send(rows, dy=s) for s in range(1, y_count)], axis=0)
    if cores == 2:
        far = send(rows, dc=1)
    else:
        far = rows
    near_sum, far_sum = branches(
        fanout, rows, far, expert_gate, expert_up, expert_down, gate_pieces, down_pieces
    )

    total = near_sum.astype(F32)
    if cores == 2:
        total = total + send(far_sum, dc=1).astype(F32)
    total = total.reshape(tp_count, y_count, z_count * sequences, block)
    narrow = total.astype(BF16)
    summed = total[0, 0]
    for t in range(tp_count):
        for y in range(y_count):
            if (t, y) != (0, 0):
                summed = summed + send(narrow[t, y], dx=-t, dy=-y).astype(F32)
    summed = summed.reshape(z_count, sequences, block)
    narrow = summed.astype(BF16)
    result = lax.dynamic_slice_in_dim(after_mix, tp_index * block, block, 1) + summed[0]
    for z in range(1, z_count):
        result = result + send(narrow[z], dz=-z).astype(F32)
    return result.astype(BF16)


def solution(mesh):
    placed = (
        P("ep", None),
        P("ep"),
        P("ep", "tp", None, None),
        P(),
        P(None, "tp"),
        P(None, "tp"),
        P(None, "tp"),
        P("tp", None),
        P(),
        P(),
        P("tp", "ep"),
        P("tp", "ep"),
        P("ep", "tp"),
        P("ep", None),
        P("ep", None),
        P("ep", None, "tp"),
        P("ep", None, "tp"),
        P("ep", "tp", None),
    )

    return jax.shard_map(
        on_device, mesh=mesh, in_specs=placed, out_specs=P("ep", "tp"), check_vma=False
    )
```

```python
import jax
import jax.numpy as jnp
import numpy as np
from jax import lax
from jax.experimental import pallas as pl
from jax.experimental.pallas import tpu as pltpu
from jax.sharding import PartitionSpec as P

EPS = 1e-06
LANES = 128
F32 = jnp.float32
BF16 = jnp.bfloat16


def dot(a, b):
    return jnp.dot(a, b, preferred_element_type=F32)


def frequencies(head_dim):
    half = head_dim // 2
    inverse = 1.0 / 10000.0 ** np.linspace(0.0, 1.0, half)
    return jnp.asarray(np.concatenate([inverse, inverse])[None, :], F32)


def turns(angle):
    whole = jnp.round(angle * (0.5 / np.pi))
    first = 6.28125
    second = float(np.float32(2 * np.pi - first).astype(jnp.bfloat16))
    third = 2 * np.pi - first - second
    rest = ((angle - whole * first) - whole * second) - whole * third
    return jnp.cos(rest), jnp.sin(rest)


def mixer_kernel(tok, gain, where, freq, wq, wk, wv, st, wo, out, q_buf, k_buf, v_buf, s_buf, o_buf, sems):
    copies = [
        pltpu.make_async_copy(src, dst, sems.at[i])
        for i, (src, dst) in enumerate(
            [(wq, q_buf), (wk, k_buf), (wv, v_buf), (st, s_buf), (wo, o_buf)]
        )
    ]
    for copy in copies:
        copy.start()
    rows, heads, head_dim = s_buf.shape[0], s_buf.shape[1], s_buf.shape[2]
    values = tok[...].astype(F32)
    scale = lax.rsqrt(jnp.mean(values * values, axis=-1, keepdims=True) + EPS)
    normed = (values * scale * gain[...]).astype(BF16)
    copies[0].wait()
    query = dot(normed, q_buf[...])
    copies[1].wait()
    key = dot(normed, k_buf[...])
    copies[2].wait()
    value = dot(normed, v_buf[...])
    half = head_dim // 2
    square = (rows, rows)
    diagonal = lax.broadcasted_iota(jnp.int32, square, 0) == lax.broadcasted_iota(
        jnp.int32, square, 1
    )
    spread = jnp.broadcast_to(where[...].astype(F32), square)
    at = jnp.sum(jnp.where(diagonal, spread, 0.0), axis=1, keepdims=True)
    cosine, sine = turns(at * freq[...])
    sine = jnp.where(lax.broadcasted_iota(jnp.int32, sine.shape, 1) < half, -sine, sine)
    all_heads = heads * lax.axis_size("tp")
    first_head = lax.axis_index("tp") * heads
    copies[3].wait()
    parts = []
    for h in range(heads):
        cols = slice(h * head_dim, (h + 1) * head_dim)
        q = query[:, cols]
        k = key[:, cols]
        q = q * cosine + pltpu.roll(q, half, 1) * sine
        k = (k * cosine + pltpu.roll(k, half, 1) * sine) * head_dim ** (-0.5)
        turned = q.T
        old = jnp.concatenate(
            [
                jnp.sum(turned[:, b : b + 1] * s_buf[b, h], axis=0, keepdims=True)
                for b in range(rows)
            ],
            axis=0,
        )
        number = jnp.full((1, head_dim), first_head + h, jnp.int32).astype(F32)
        decay = 1.0 - jnp.exp2(-5.0 - 5.0 * number / (all_heads - 1))
        got = decay * old + jnp.sum(q * k, axis=-1, keepdims=True) * value[:, cols]
        got = got * lax.rsqrt(jnp.mean(got * got, axis=-1, keepdims=True) + EPS)
        parts.append(got.astype(BF16))
    retrieved = parts[0] if heads == 1 else jnp.concatenate(parts, axis=1)
    copies[4].wait()
    out[...] = dot(retrieved, o_buf[...]).astype(BF16)


def mixer(tokens, gain, positions, freq, wq, wk, wv, state, wo):
    vmem = pl.BlockSpec(memory_space=pltpu.VMEM)
    hbm = pl.BlockSpec(memory_space=pl.ANY)
    return pl.pallas_call(
        mixer_kernel,
        out_shape=jax.ShapeDtypeStruct(tokens.shape, BF16),
        in_specs=[vmem] * 4 + [hbm] * 5,
        out_specs=vmem,
        scratch_shapes=[pltpu.VMEM(a.shape, a.dtype) for a in (wq, wk, wv, state, wo)]
        + [pltpu.SemaphoreType.DMA((5,))],
        name="mixer",
    )(tokens, gain, positions, freq, wq, wk, wv, state, wo)


def norm_kernel(fanout, tok, gain, gate, meta, *refs):
    parts, (rows_out, mix_out) = refs[:-2], refs[-2:]
    width = tok.shape[1]
    mixed = parts[0][...].astype(F32)
    for part in parts[1:]:
        mixed = mixed + part[...].astype(F32)
    after = tok[...].astype(F32) + mixed
    mix_out[...] = after
    scale = lax.rsqrt(jnp.mean(after * after, axis=-1, keepdims=True) + EPS)
    ffn = (after * scale * gain[...]).astype(BF16)
    rows_out[:, :width] = ffn
    logit = jnp.sum(ffn.astype(F32) * gate[...].astype(F32), axis=-1, keepdims=True)
    branch = 1.0 / (1.0 + jnp.exp(-logit))
    high = branch.astype(BF16).astype(F32)
    low = branch - high
    info = meta[...].astype(F32)
    lane = lax.broadcasted_iota(jnp.int32, info.shape, 1)
    info = jnp.where(lane == 3 * fanout, high, info)
    info = jnp.where(lane == 3 * fanout + 1, low, info)
    rows_out[:, width:] = info.astype(BF16)


def norm_rows(fanout, tokens, gain, gate, meta, parts):
    vmem = pl.BlockSpec(memory_space=pltpu.VMEM)
    rows, width = tokens.shape
    return pl.pallas_call(
        lambda *refs: norm_kernel(fanout, *refs),
        out_shape=(
            jax.ShapeDtypeStruct((rows, width + LANES), BF16),
            jax.ShapeDtypeStruct((rows, width), F32),
        ),
        in_specs=[vmem] * (4 + len(parts)),
        out_specs=(vmem, vmem),
        compiler_params=pltpu.CompilerParams(vmem_limit_bytes=8 * 1024 * 1024),
        name="norm",
    )(in_vmem(tokens), gain, gate, meta, *[in_vmem(part) for part in parts])


def silu(v):
    return v / (1.0 + jnp.exp(-v))


def branch_kernel(tp_count, fanout, src, eg, eu, ed, *refs):
    pieces = refs[: 2 * tp_count]
    dst = refs[2 * tp_count]
    eg_buf, eu_buf, ed_buf = eg, eu, ed
    dg_bufs, dd_bufs = pieces[:tp_count], pieces[tp_count:]
    width = eg_buf.shape[1]
    block = width // tp_count
    units = dd_bufs[0].shape[0]
    per_device = eg_buf.shape[0]
    ep_index = lax.axis_index("ep")
    tp_index = lax.axis_index("tp")
    spots = [lax.rem(tp_index - t + tp_count, tp_count) * block for t in range(tp_count)]
    spots = [pl.multiple_of(s, LANES) for s in spots]
    rows = src.shape[0]
    step = min(rows, 256)

    def work(start):
        at = pl.ds(start, step)
        info = src[at, width:].astype(F32)
        lane = lax.broadcasted_iota(jnp.int32, info.shape, 1)
        high = pltpu.roll(info, LANES - fanout, 1)
        low = pltpu.roll(info, LANES - 2 * fanout, 1)
        branch = jnp.sum(
            jnp.where((lane >= 3 * fanout) & (lane < 3 * fanout + 2), info, 0.0),
            axis=1,
            keepdims=True,
        )
        x = src[at, :width]
        hidden = []
        for k in range(per_device):
            own = (ep_index * per_device + k).astype(F32)
            weight = jnp.sum(
                jnp.where((lane < fanout) & (info == own), high + low, 0.0), axis=1, keepdims=True
            )
            gate = dot(x, eg_buf[k])
            hidden.append((silu(gate) * dot(x, eu_buf[k]) * weight).astype(BF16))
        both = dot(src[at, pl.ds(spots[0], block)], dg_bufs[0][...])
        for t in range(1, tp_count):
            both = both + dot(src[at, pl.ds(spots[t], block)], dg_bufs[t][...])
        dense = (silu(both[:, :units]) * both[:, units:] * branch).astype(BF16)
        for t in range(tp_count):
            total = dot(dense, dd_bufs[t][...])
            for k in range(per_device):
                total = total + dot(hidden[k], ed_buf[k, :, pl.ds(spots[t], block)])
            dst[t, at, :] = total.astype(BF16)

    if rows == step:
        work(0)
    else:

        def body(i, carry):
            work(pl.multiple_of(i * step, step))
            return carry

        lax.fori_loop(0, rows // step, body, 0)


def in_vmem(a):
    return pltpu.with_memory_space_constraint(a, pltpu.VMEM)


def branches(fanout, rows, eg, eu, ed, gate_pieces, down_pieces):
    vmem = pl.BlockSpec(memory_space=pltpu.VMEM)
    tp_count = len(gate_pieces)
    shape = (tp_count, rows.shape[0], eg.shape[1] // tp_count)
    args = [in_vmem(a) for a in (rows, eg, eu, ed, *gate_pieces, *down_pieces)]
    return pl.pallas_call(
        lambda *refs: branch_kernel(tp_count, fanout, *refs),
        out_shape=jax.ShapeDtypeStruct(shape, BF16),
        in_specs=[vmem] * len(args),
        out_specs=vmem,
        compiler_params=pltpu.CompilerParams(vmem_limit_bytes=24 * 1024 * 1024),
        name="branches",
    )(*args)


def on_device(
    tokens,
    positions,
    state,
    mix_gain,
    w_query,
    w_key,
    w_value,
    w_out,
    ffn_gain,
    branch_gate,
    dense_gate,
    dense_up,
    dense_down,
    routes,
    route_scores,
    expert_gate,
    expert_up,
    expert_down,
):
    sequences, width = tokens.shape
    tp_count = lax.axis_size("tp")
    ep_count = lax.axis_size("ep")
    tp_index = lax.axis_index("tp")
    fanout = routes.shape[1]
    block = width // tp_count
    cores = 2 if ep_count % 2 == 0 else 1
    chips = ep_count // cores
    y_count = 1
    while chips % (y_count * 2) == 0 and (y_count * 2) ** 2 <= chips:
        y_count *= 2
    z_count = chips // y_count

    def send(x, dz=0, dy=0, dc=0, dx=0):
        pairs = []
        for z in range(z_count):
            for y in range(y_count):
                for c in range(cores):
                    for q in range(tp_count):
                        src = ((z * y_count + y) * cores + c) * tp_count + q
                        to_z, to_y = (z + dz) % z_count, (y + dy) % y_count
                        to_c, to_q = (c + dc) % cores, (q + dx) % tp_count
                        dst = ((to_z * y_count + to_y) * cores + to_c) * tp_count + to_q
                        pairs.append((src, dst))
        return lax.ppermute(x, ("ep", "tp"), pairs)

    partial_out = mixer(
        tokens,
        mix_gain[None, :],
        positions[None, :],
        frequencies(state.shape[2]),
        w_query,
        w_key,
        w_value,
        state,
        w_out,
    )
    parts = [partial_out] + [send(partial_out, dx=s) for s in range(1, tp_count)]

    route_weights = route_scores / jnp.sum(route_scores, axis=1, keepdims=True)
    high = lax.reduce_precision(route_weights, 8, 7)
    low = route_weights - high
    meta = jnp.concatenate([routes.astype(F32), high, low], axis=1)
    meta = jnp.pad(meta, ((0, 0), (0, LANES - meta.shape[1]))).astype(BF16)
    payload, after_mix = norm_rows(
        fanout, tokens, ffn_gain[None, :], branch_gate[None, :], meta, parts
    )

    units = dense_gate.shape[1] // tp_count

    def gate_piece(index):
        at = lax.rem(index, tp_count) * units
        return jnp.concatenate(
            [
                lax.dynamic_slice_in_dim(dense_gate, at, units, 1),
                lax.dynamic_slice_in_dim(dense_up, at, units, 1),
            ],
            axis=1,
        )

    def down_piece(index):
        return lax.dynamic_slice_in_dim(dense_down, lax.rem(index, tp_count) * units, units, 0)

    gate_pieces = [gate_piece(tp_index)]
    down_pieces = [down_piece(tp_index)]
    for s in range(1, tp_count):
        there_gate, there_down, _ = lax.optimization_barrier(
            (gate_piece(tp_index + s), down_piece(tp_index + s), parts[s])
        )
        gate_pieces.append(send(there_gate, dx=s))
        down_pieces.append(send(there_down, dx=s))

    rows = jnp.concatenate([payload] + [send(payload, dz=s) for s in range(1, z_count)], axis=0)
    rows = jnp.concatenate([rows] + [send(rows, dy=s) for s in range(1, y_count)], axis=0)
    weights = (expert_gate, expert_up, expert_down, gate_pieces, down_pieces)
    near_sum = branches(fanout, rows, *weights)
    if cores == 2:
        far = send(rows, dc=1)
        back = send(branches(fanout, far, *weights), dc=1)

    reach = z_count * sequences

    def chip_sum(t, y):
        at = slice(y * reach, (y + 1) * reach)
        total = near_sum[t, at].astype(F32)
        if cores == 2:
            total = total + back[t, at].astype(F32)
        return total.astype(BF16)

    pieces = [
        send(chip_sum(t, y), dx=-t, dy=-y) if (t, y) != (0, 0) else chip_sum(t, y)
        for t in range(tp_count)
        for y in range(y_count)
    ]

    def plane_sum(z):
        at = slice(z * sequences, (z + 1) * sequences)
        total = pieces[0][at].astype(F32)
        for piece in pieces[1:]:
            total = total + piece[at].astype(F32)
        return total

    result = lax.dynamic_slice_in_dim(after_mix, tp_index * block, block, 1) + plane_sum(0)
    for z in range(1, z_count):
        result = result + send(plane_sum(z).astype(BF16), dz=-z).astype(F32)
    return result.astype(BF16)


def solution(mesh):
    placed = (
        P("ep", None),
        P("ep"),
        P("ep", "tp", None, None),
        P(),
        P(None, "tp"),
        P(None, "tp"),
        P(None, "tp"),
        P("tp", None),
        P(),
        P(),
        P("tp", "ep"),
        P("tp", "ep"),
        P("ep", "tp"),
        P("ep", None),
        P("ep", None),
        P("ep", None, "tp"),
        P("ep", None, "tp"),
        P("ep", "tp", None),
    )

    return jax.shard_map(
        on_device, mesh=mesh, in_specs=placed, out_specs=P("ep", "tp"), check_vma=False
    )
```
